32 devices in a mesh: ep: 8 (over z, y), tp: 4 (over x, core).
Axes of the slice: x: 2, y: 2, z: 4, core: 2. Of those that a mesh axis runs over, the one named last changes fastest.
Arguments:
- query: bfloat16 [8192, 1024], P('ep', 'tp'), may hold values from -6 to 6
- keys: bfloat16 [8192, 1024], P('ep', 'tp'), may hold values from -6 to 6
- values: bfloat16 [8192, 2048], P('ep', 'tp'), may hold values from -6 to 6
- gate_pre: bfloat16 [8192, 2048], P('ep', 'tp'), may hold values from -6 to 6
- log_decay: float32 [16, 8192], P('tp', 'ep'), may hold values from -1 to 0
- out_weight: bfloat16 [2048, 4096], P(None, 'tp'), may hold values from -0.125 to 0.125
- expert_input: bfloat16 [2048, 4096], P(('ep', 'tp')), may hold values from -6 to 6
- norm_gain: float32 [4096], replicated, may hold values from 0.1 to 1.9
- routes: int32 [2048, 2], P(('ep', 'tp')), may hold values from 0 to 7, all different within a row; in each aligned block of 64 rows (0 to 63, 64 to 127, ...) at most 24 rows name the same one
- route_weights: float32 [2048, 2], P(('ep', 'tp')), may hold values from 0.1 to 1
- w_gate: bfloat16 [8, 4096, 1536], P('ep', None, 'tp'), may hold values from -0.09375 to 0.09375
- w_up: bfloat16 [8, 4096, 1536], P('ep', None, 'tp'), may hold values from -0.09375 to 0.09375
- w_down: bfloat16 [8, 1536, 4096], P('ep', 'tp'), may hold values from -0.15625 to 0.15625
Outputs:
- mixed: bfloat16 [8192, 4096], P('ep', 'tp')
- moe_out: bfloat16 [2048, 4096], P(('ep', 'tp'))
The draws below stay inside these ranges and needn't reach their ends.
Inputs may be any that keep to these rules, and one draw needn't show every extreme that they name: `routes`: each row names 2 different experts; among the rows of one device no expert is named by more than 24 rows, a bound that some block reaches of some device.
All inputs are finite; a program needn't handle non-finite values.
Results may differ from the reference program's by a relative error of at most 0.018.
Values may be sent and summed in bfloat16 or wider, within the bound.
A program may use at most 128 MiB of HBM per device.

```python
import math
import jax
import jax.numpy as jnp
import numpy as np
from jax import lax

D = 4096
RETENTION_HEADS = 16
DK = 64
DV = 128
FFE = 1536
TOP = 2
BLK = 128
TB_DEV = 64
EXPERTS = 8
CAP = 24
ROWS_A = 1024
FIRST_TOKENS = 8192
TOKENS_B = 2048
N_EP = 8
N_TP = 4


def draw_log_decay(key, part):
    key_sequence = jax.random.split(jax.random.fold_in(key, 71), 7)
    fast_share = 0.5
    fast_heads = jax.random.uniform(key_sequence[0], (RETENTION_HEADS,), jnp.float32) < fast_share
    fast_rate = jnp.exp(jax.random.uniform(key_sequence[1], (RETENTION_HEADS,), jnp.float32, jnp.log(1.0 / 80.0), jnp.log(1.0 / 30.0)))
    slow_rate = jax.random.uniform(key_sequence[2], (RETENTION_HEADS,), jnp.float32, 0.3, 0.8) / FIRST_TOKENS
    base_rate = jnp.where(fast_heads, fast_rate, slow_rate)
    span_len = max(ROWS_A // 2, 1)
    span_count = FIRST_TOKENS // span_len
    span_factor = jnp.exp(jax.random.uniform(key_sequence[3], (RETENTION_HEADS, span_count), jnp.float32, jnp.log(0.4), jnp.log(2.5)))
    span_factor = jnp.repeat(span_factor, span_len, axis=1)
    roughness = jnp.exp(jax.random.uniform(key_sequence[4], (RETENTION_HEADS, FIRST_TOKENS), jnp.float32, -0.5, 0.5))
    logarithm_rate = -(base_rate[:, None] * span_factor * roughness)
    spike_position = jax.random.randint(key_sequence[5], (3,), 0, FIRST_TOKENS)
    spike_strength = jnp.log(jax.random.uniform(key_sequence[6], (RETENTION_HEADS, 3), jnp.float32, 0.5, 0.8))
    position_index = jnp.arange(FIRST_TOKENS, dtype=jnp.int32)
    expert_hits = (position_index[None, :] == spike_position[:, None]).astype(jnp.float32)
    decay_spikes = jnp.dot(spike_strength, expert_hits)
    return (logarithm_rate + decay_spikes).astype(jnp.float32)


def steps_of(key, extent, cuts, low, high):
    gain, own = 1.0, jax.random.fold_in(key, 6)
    for axis_at, blocks in cuts:
        steps = jnp.exp(jax.random.uniform(jax.random.fold_in(own, axis_at), (blocks,), jnp.float32, low / len(cuts), high / len(cuts)))
        gain = gain * jnp.repeat(steps, extent[axis_at] // blocks).reshape([-1 if axis == axis_at else 1 for axis in range(len(extent))])
    return gain


def deal_out(stream_key, own, number, rows, count, top, most, slope):
    order = jax.random.permutation(stream_key, count)
    crowded, common = portions_of(count, rows * top, most, slope, True), portions_of(count, rows * top, most, slope, False)
    places = jnp.arange(count)

    def named(tallies, offset_by):
        used = int((tallies > 0).sum())
        fixed = max(1, used // 4)
        passed = fixed + (places - fixed + offset_by * (used - fixed)) % max(1, count - fixed)
        return jnp.zeros((count,), jnp.int32).at[order[jnp.where(places < fixed, places, passed)]].set(jnp.asarray(tallies, jnp.int32))

    tallies = jnp.where(number % 4 == 0, named(crowded, number // 4), named(common, number - number // 4 - 1))
    mixed = jax.random.permutation(jax.random.fold_in(own, 3), count)
    donor, sink = mixed[0:count // 2 * 2:2], mixed[1:count // 2 * 2:2]
    slack = jnp.minimum(tallies[donor] - 1, most - tallies[sink]) // 2
    slack = jnp.where((donor == order[0]) | (sink == order[0]) | (tallies[sink] == 0), 0, jnp.maximum(slack, 0))
    passed = jax.random.randint(jax.random.fold_in(own, 4), (count // 2,), 0, 1 << 20) % (slack + 1)
    tallies = tallies.at[donor].add(-passed).at[sink].add(passed)
    items = jnp.searchsorted(jnp.cumsum(tallies), jnp.arange(rows * top), side="right").astype(jnp.int32)
    listing = items.reshape(top, rows).T
    listing = listing[jax.random.permutation(jax.random.fold_in(own, 1), rows)]
    offset_by = jax.random.randint(jax.random.fold_in(own, 2), (rows, 1), 0, top)
    return jnp.take_along_axis(listing, (jnp.arange(top)[None, :] + offset_by) % top, axis=1)


def portions_of(number_of, total, bound, lean, full):
    weights = [(1 << 20) // math.isqrt(rank ** lean) + 1 for rank in range(1, number_of + 1)]
    largest = bound if full else min(bound, max(-(-total // number_of), total * weights[0] // sum(weights)))
    least = 1 if total - largest >= number_of - 1 else 0
    given, surplus = [largest] + [least] * (number_of - 1), total - largest - least * (number_of - 1)
    while surplus > 0:
        candidates = [i for i in range(1, number_of) if given[i] < largest] or [i for i in range(1, number_of) if given[i] < bound]
        whole, left = sum([weights[i] for i in candidates]), surplus
        for i in candidates:
            more = min(bound - given[i], max(1, left * weights[i] // whole), surplus)
            given[i] = given[i] + more
            surplus = surplus - more
    return np.array(given)


def noise(rng, shape, deviation, reach, cuts=(), kind=jnp.bfloat16):
    factor_of = steps_of(rng, shape, cuts, -0.22, 0.18) if cuts else 1.0
    values = jax.random.normal(rng, shape, jnp.float32) * deviation * factor_of
    return jnp.minimum(jnp.maximum(values, -reach), reach).astype(kind)


def setup_inputs(seed: int = 0) -> dict:
    arg_keys = jax.random.split(jax.random.key(seed), 14)
    query = noise(arg_keys[0], (FIRST_TOKENS, RETENTION_HEADS * DK), 1.0, 6.0, ((0, 8), (1, 4)))
    keys = noise(arg_keys[1], (FIRST_TOKENS, RETENTION_HEADS * DK), 1.0, 6.0, ((0, 8), (1, 4)))
    values = noise(arg_keys[2], (FIRST_TOKENS, RETENTION_HEADS * DV), 1.0, 6.0, ((0, 8), (1, 4)))
    gate_pre = noise(arg_keys[3], (FIRST_TOKENS, RETENTION_HEADS * DV), 1.0, 6.0, ((0, 8), (1, 4)))
    log_decay = draw_log_decay(jax.random.fold_in(arg_keys[13], 71), 0)
    out_weight = noise(arg_keys[5], (RETENTION_HEADS * DV, D), (RETENTION_HEADS * DV) ** -0.5, 0.125, ((1, 4),))
    expert_input = noise(arg_keys[6], (TOKENS_B, D), 1.0, 6.0, ((0, 32),))
    norm_gain = jnp.clip(1.0 + 0.18 * jax.random.normal(arg_keys[7], (D,), jnp.float32), 0.1, 1.9)
    routes_keys = jax.random.split(jax.random.fold_in(arg_keys[8], 1), TOKENS_B // TB_DEV)
    routes_turns = jax.random.permutation(jax.random.fold_in(arg_keys[8], 3), TOKENS_B // TB_DEV)
    routes = jax.vmap(lambda own, number: deal_out(jax.random.fold_in(arg_keys[8], 2), own, number, TB_DEV, EXPERTS, TOP, CAP, 1))(routes_keys, routes_turns).reshape((TOKENS_B, TOP))
    route_weights = jnp.clip(0.1 + 0.9 * jax.random.uniform(arg_keys[9], (TOKENS_B, TOP), jnp.float32) ** steps_of(arg_keys[9], (TOKENS_B, TOP), ((0, 32),), -0.2, 0.2), 0.1, 1.0)
    w_gate = noise(arg_keys[10], (EXPERTS, D, FFE), D ** -0.5, 0.09375, ((0, 8), (2, 4)))
    w_up = noise(arg_keys[11], (EXPERTS, D, FFE), D ** -0.5, 0.09375, ((0, 8), (2, 4)))
    w_down = noise(arg_keys[12], (EXPERTS, FFE, D), FFE ** -0.5, 0.15625, ((0, 8), (1, 4)))
    return {"query": query, "keys": keys, "values": values, "gate_pre": gate_pre, "log_decay": log_decay, "out_weight": out_weight, "expert_input": expert_input, "norm_gain": norm_gain, "routes": routes, "route_weights": route_weights, "w_gate": w_gate, "w_up": w_up, "w_down": w_down}


def rotate(vectors, position_index):
    half_dim = vectors.shape[-1] // 2
    inverse = 1.0 / 10000.0 ** jnp.linspace(0.0, 1.0, half_dim, dtype=jnp.float32)
    angles = position_index[:, None] * inverse[None, :]
    cosine = jnp.cos(angles)[:, None, :]
    sine_part = jnp.sin(angles)[:, None, :]
    first_half = vectors[..., :half_dim]
    second_half = vectors[..., half_dim:]
    return jnp.concatenate([first_half * cosine - second_half * sine_part, first_half * sine_part + second_half * cosine], axis=-1)

def retention_block(state, inputs):
    query_blk, key_blk, value_blk, decay_blk = inputs
    width_blk = decay_blk.shape[1]
    running = jnp.cumsum(decay_blk, axis=1)
    spread = running[:, :, None] - running[:, None, :]
    causal = jnp.tril(jnp.ones((width_blk, width_blk), dtype=bool))[None]
    weights = jnp.where(causal, jnp.exp(jnp.where(causal, spread, 0.0)), 0.0)
    highest = lax.Precision.HIGHEST
    scores = jnp.einsum('hid,hjd->hij', query_blk, key_blk, precision=highest) * weights
    output = jnp.einsum('hij,hje->hie', scores, value_blk, precision=highest)
    output = output + jnp.einsum('hid,hde->hie', query_blk * jnp.exp(running)[:, :, None], state, precision=highest)
    closing = running[:, -1:]
    state_next = state * jnp.exp(closing)[:, :, None] + jnp.einsum('hjd,hje->hde', key_blk * jnp.exp(closing - running)[:, :, None], value_blk, precision=highest)
    return (state_next, output)

def head_norm(vectors):
    centered = vectors - lax.optimization_barrier(jnp.mean(vectors, axis=-1, keepdims=True))
    variance = lax.optimization_barrier(jnp.mean(centered * centered, axis=-1, keepdims=True))
    return centered * lax.rsqrt(variance + 1e-06)

def mixer(query, keys, values, gate_pre, log_decay, out_weight):
    length = query.shape[0]
    position_index = jnp.arange(length, dtype=jnp.int32).astype(jnp.float32)
    rotated_q = rotate(query.astype(jnp.float32).reshape(length, RETENTION_HEADS, DK), position_index)
    rotated_k = rotate(keys.astype(jnp.float32).reshape(length, RETENTION_HEADS, DK), position_index) * DK ** (-0.5)
    value_rows = values.astype(jnp.float32).reshape(length, RETENTION_HEADS, DV)
    block_count = length // BLK

    def to_blocks(array):
        return array.reshape(block_count, BLK, RETENTION_HEADS, array.shape[-1]).transpose(0, 2, 1, 3)
    decay_blocks = log_decay.reshape(RETENTION_HEADS, block_count, BLK).transpose(1, 0, 2)
    start_state = jnp.zeros((RETENTION_HEADS, DK, DV), jnp.float32)
    final_state, outputs = lax.scan(retention_block, start_state, (to_blocks(rotated_q), to_blocks(rotated_k), to_blocks(value_rows), decay_blocks))
    combined = outputs.transpose(0, 2, 1, 3).reshape(length, RETENTION_HEADS, DV)
    gate_act = jax.nn.silu(gate_pre.astype(jnp.float32).reshape(length, RETENTION_HEADS, DV))
    gated = (gate_act * head_norm(combined)).reshape(length, RETENTION_HEADS * DV).astype(jnp.bfloat16)
    return jnp.dot(gated, out_weight, preferred_element_type=jnp.float32).astype(jnp.bfloat16)

def experts(expert_input, norm_gain, routes, route_weights, w_gate, w_up, w_down):
    rows_f = expert_input.astype(jnp.float32)
    centered = rows_f - lax.optimization_barrier(jnp.mean(rows_f, axis=-1, keepdims=True))
    variance = lax.optimization_barrier(jnp.mean(centered * centered, axis=-1, keepdims=True))
    normed = (centered * lax.rsqrt(variance + 1e-05) * norm_gain).astype(jnp.bfloat16)
    pair_count = TOKENS_B * TOP
    expert_ids = routes.reshape(pair_count).astype(jnp.int32)
    limit = N_EP * N_TP * CAP
    block_width = FFE // N_TP

    def one_expert(pair_out, index):
        chosen = jnp.nonzero(expert_ids == index, size=limit, fill_value=pair_count)[0].astype(jnp.int32)
        token_rows = jnp.minimum(chosen // TOP, TOKENS_B - 1).astype(jnp.int32)
        rows_in = normed[token_rows]
        gate_w = lax.dynamic_index_in_dim(w_gate, index, 0, keepdims=False)
        up_w = lax.dynamic_index_in_dim(w_up, index, 0, keepdims=False)
        down_w = lax.dynamic_index_in_dim(w_down, index, 0, keepdims=False)
        hidden = (jax.nn.silu(jnp.dot(rows_in, gate_w, preferred_element_type=jnp.float32)) * jnp.dot(rows_in, up_w, preferred_element_type=jnp.float32)).astype(jnp.bfloat16)
        total = jnp.zeros((limit, D), jnp.float32)
        for part_index in range(N_TP):
            lower = part_index * block_width
            part_rows = jnp.dot(hidden[:, lower:lower + block_width], down_w[lower:lower + block_width], preferred_element_type=jnp.float32).astype(jnp.bfloat16)
            total = total + lax.optimization_barrier(part_rows).astype(jnp.float32)
        pair_out = pair_out.at[chosen].set(total.astype(jnp.bfloat16), mode='drop')
        return (pair_out, None)
    pair_out, _ = lax.scan(one_expert, jnp.zeros((pair_count, D), jnp.bfloat16), jnp.arange(EXPERTS, dtype=jnp.int32))
    weighted = pair_out.reshape(TOKENS_B, TOP, D).astype(jnp.float32) * route_weights[:, :, None]
    return lax.optimization_barrier(jnp.sum(weighted, axis=1)).astype(jnp.bfloat16)

def reference(query, keys, values, gate_pre, log_decay, out_weight, expert_input, norm_gain, routes, route_weights, w_gate, w_up, w_down):
    mixed = mixer(query, keys, values, gate_pre, log_decay, out_weight)
    moe_out = experts(expert_input, norm_gain, routes, route_weights, w_gate, w_up, w_down)
    return (mixed, moe_out)
```

```python
import functools
import jax
import jax.numpy as jnp
from jax import lax
from jax.experimental import pallas as pl
from jax.experimental.pallas import tpu as pltpu
from jax.sharding import PartitionSpec as P

BF = jnp.bfloat16
F32 = jnp.float32
VM = pltpu.VMEM


def cost(flops, moved, trans=0):
    return pl.CostEstimate(flops=int(flops), bytes_accessed=int(moved), transcendentals=int(trans))


def params(mib=48, **more):
    return pltpu.CompilerParams(vmem_limit_bytes=mib * 1024 * 1024, **more)


def swap(array, axis, bit):
    size = lax.axis_size(axis)
    return lax.ppermute(array, axis, [(i, i ^ bit) for i in range(size)])


def shift(array, axis, step):
    size = lax.axis_size(axis)
    return lax.ppermute(array, axis, [(i, (i + step) % size) for i in range(size)])


def turn(x, cos_ref, sin_ref, head_dim):
    width = x.shape[1]
    half = head_dim // 2
    lane = lax.broadcasted_iota(jnp.int32, x.shape, 1)
    first = lane % head_dim < half
    other = jnp.where(first, pltpu.roll(x, width - half, 1), pltpu.roll(x, half, 1))
    reps = width // cos_ref.shape[1]
    cos = jnp.concatenate([cos_ref[...]] * reps, axis=1)
    sin = jnp.concatenate([sin_ref[...]] * reps, axis=1)
    return x * cos + other * sin


def next_state(state, kt, value, run_row, closing):
    scaled = (kt * jnp.exp(closing - run_row)).astype(BF)
    return state * jnp.exp(closing) + jnp.dot(scaled, value, preferred_element_type=F32)


def state_kernel(heads, dk, dv, k_ref, v_ref, cos_ref, sin_ref, run_ref, out_ref, state, total):
    b = pl.program_id(0)

    @pl.when(b == 0)
    def _():
        state[...] = jnp.zeros_like(state)
        total[...] = jnp.zeros_like(total)

    kt = (turn(k_ref[...].astype(F32), cos_ref, sin_ref, dk) * dk ** (-0.5)).T
    width = run_ref.shape[2]
    for h in range(heads):
        run_row = run_ref[0, h : h + 1, :]
        closing = run_row[:, width - 1 : width]
        rows = slice(h * dk, (h + 1) * dk)
        state[rows, :] = next_state(
            state[rows, :], kt[rows, :], v_ref[:, h * dv : (h + 1) * dv], run_row, closing
        )
        total[h : h + 1, :] = total[h : h + 1, :] + closing

    @pl.when(b == pl.num_programs(0) - 1)
    def _():
        out_ref[0 : heads * dk, :] = state[...].astype(BF)
        out_ref[heads * dk :, :] = jnp.exp(total[...]).astype(BF)


def mix_kernel(
    heads, dk, dv, q_ref, k_ref, v_ref, g_ref, cos_ref, sin_ref, run_ref, runt_ref, in_ref, out_ref, state
):
    b = pl.program_id(0)

    @pl.when(b == 0)
    def _():
        state[...] = in_ref[...]

    q = turn(q_ref[...].astype(F32), cos_ref, sin_ref, dk)
    kt = (turn(k_ref[...].astype(F32), cos_ref, sin_ref, dk) * dk ** (-0.5)).T
    ktb = kt.astype(BF)
    width = q.shape[0]
    row = lax.broadcasted_iota(jnp.int32, (width, width), 0)
    col = lax.broadcasted_iota(jnp.int32, (width, width), 1)
    causal = row >= col
    for h in range(heads):
        run_row = run_ref[0, h : h + 1, :]
        run_col = runt_ref[:, h : h + 1]
        closing = run_row[:, width - 1 : width]
        rows = slice(h * dk, (h + 1) * dk)
        qh = q[:, rows]
        vh = v_ref[:, h * dv : (h + 1) * dv]
        weights = jnp.where(causal, jnp.exp(jnp.where(causal, run_col - run_row, 0.0)), 0.0)
        scores = jnp.dot(qh.astype(BF), ktb[rows, :], preferred_element_type=F32) * weights
        out = jnp.dot(scores.astype(BF), vh, preferred_element_type=F32)
        carried = state[rows, :]
        out = out + jnp.dot(
            (qh * jnp.exp(run_col)).astype(BF), carried.astype(BF), preferred_element_type=F32
        )
        state[rows, :] = next_state(carried, kt[rows, :], vh, run_row, closing)
        centered = out - jnp.mean(out, axis=-1, keepdims=True)
        variance = jnp.mean(centered * centered, axis=-1, keepdims=True)
        gate = g_ref[:, h * dv : (h + 1) * dv].astype(F32)
        act = gate / (1.0 + jnp.exp(-gate))
        out_ref[:, h * dv : (h + 1) * dv] = (act * (centered * lax.rsqrt(variance + 1e-06))).astype(BF)


def project_kernel(where_ref, a_ref, b_ref, c_ref, d_ref, w_ref, out_ref):
    depth = a_ref.shape[1]
    total = None
    for j, ref in enumerate((a_ref, b_ref, c_ref, d_ref)):
        start = pl.multiple_of(where_ref[j] * depth, depth)
        term = jnp.dot(ref[...], w_ref[pl.ds(start, depth), :], preferred_element_type=F32)
        total = term if total is None else total + term
    out_ref[...] = total.astype(BF)


def mixer_tables(rows, dk, log_decay, block):
    heads = log_decay.shape[0]
    offset = lax.axis_index("ep") * rows
    position = (offset + jnp.arange(rows, dtype=jnp.int32)).astype(F32)
    inverse = 1.0 / 10000.0 ** jnp.linspace(0.0, 1.0, dk // 2, dtype=F32)
    angles = position[:, None] * inverse[None, :]
    cos = jnp.cos(angles)
    sin = jnp.sin(angles)
    reps = 128 // dk
    cos = jnp.concatenate([cos, cos] * reps, axis=1)
    sin = jnp.concatenate([-sin, sin] * reps, axis=1)
    run = jnp.cumsum(log_decay.reshape(heads, rows // block, block), axis=2)
    return cos, sin, run.transpose(1, 0, 2), run.reshape(heads, rows).T


def mixer_state(keys, values, cos, sin, run, block):
    rows = keys.shape[0]
    heads = run.shape[1]
    dk, dv = keys.shape[1] // heads, values.shape[1] // heads
    by_row = lambda b: (b, 0)
    return pl.pallas_call(
        functools.partial(state_kernel, heads, dk, dv),
        grid=(rows // block,),
        in_specs=[
            pl.BlockSpec((block, heads * dk), by_row),
            pl.BlockSpec((block, heads * dv), by_row),
            pl.BlockSpec((block, cos.shape[1]), by_row),
            pl.BlockSpec((block, cos.shape[1]), by_row),
            pl.BlockSpec((1, heads, block), lambda b: (b, 0, 0)),
        ],
        out_specs=pl.BlockSpec((heads * dk + 16, dv), lambda b: (0, 0)),
        out_shape=jax.ShapeDtypeStruct((heads * dk + 16, dv), BF),
        scratch_shapes=[VM((heads * dk, dv), F32), VM((16, dv), F32)],
        compiler_params=params(16),
        cost_estimate=cost(2 * rows * heads * dk * dv, 4 << 20),
    )(keys, values, cos, sin, run)


def incoming_state(packed, heads):
    count = lax.axis_size("ep")
    size = packed.shape[0] - 16
    dk = size // heads
    state = jnp.zeros((heads, dk, packed.shape[1]), F32)
    factor = jnp.ones((heads, 1, packed.shape[1]), F32)
    parts = []
    for d in range(1, count):
        parts.append(lax.ppermute(packed, "ep", [(i, i + d) for i in range(count - d)]))
    for part in parts:
        state = state + factor * part[:size].astype(F32).reshape(heads, dk, -1)
        factor = factor * part[size : size + heads].astype(F32)[:, None, :]
    return state.reshape(size, packed.shape[1])


def mixer_gated(query, keys, values, gate_pre, cos, sin, run, runt, incoming, block):
    rows = keys.shape[0]
    heads = run.shape[1]
    dk, dv = keys.shape[1] // heads, values.shape[1] // heads
    by_row = lambda b: (b, 0)
    return pl.pallas_call(
        functools.partial(mix_kernel, heads, dk, dv),
        grid=(rows // block,),
        in_specs=[
            pl.BlockSpec((block, heads * dk), by_row),
            pl.BlockSpec((block, heads * dk), by_row),
            pl.BlockSpec((block, heads * dv), by_row),
            pl.BlockSpec((block, heads * dv), by_row),
            pl.BlockSpec((block, cos.shape[1]), by_row),
            pl.BlockSpec((block, cos.shape[1]), by_row),
            pl.BlockSpec((1, heads, block), lambda b: (b, 0, 0)),
            pl.BlockSpec((block, heads), by_row),
            pl.BlockSpec((heads * dk, dv), lambda b: (0, 0)),
        ],
        out_specs=pl.BlockSpec((block, heads * dv), by_row),
        out_shape=jax.ShapeDtypeStruct((rows, heads * dv), BF),
        scratch_shapes=[VM((heads * dk, dv), F32)],
        compiler_params=params(24),
        cost_estimate=cost(6e9, 8 << 20),
    )(query, keys, values, gate_pre, cos, sin, run, runt, incoming)


def project(gated, out_weight):
    half = lax.axis_size("tp") // 2
    me = lax.axis_index("tp")
    far = swap(gated, "tp", half)
    near = swap(gated, "tp", 1)
    both = swap(far, "tp", 1)
    where = jnp.stack([me, me ^ half, me ^ 1, me ^ half ^ 1]).astype(jnp.int32)
    rows, depth = gated.shape
    width = out_weight.shape[1]
    tile = 256
    spec = pl.BlockSpec((tile, depth), lambda i, where: (i, 0))
    return pl.pallas_call(
        project_kernel,
        grid_spec=pltpu.PrefetchScalarGridSpec(
            num_scalar_prefetch=1,
            grid=(rows // tile,),
            in_specs=[spec] * 4 + [pl.BlockSpec(out_weight.shape, lambda i, where: (0, 0))],
            out_specs=pl.BlockSpec((tile, width), lambda i, where: (i, 0)),
        ),
        out_shape=jax.ShapeDtypeStruct((rows, width), BF),
        compiler_params=params(32),
        cost_estimate=cost(2 * rows * depth * 4 * width, 12 << 20),
    )(where, gated, far, near, both, out_weight)


def prep_kernel(count, capacity, rel_ref, rw_ref, own_ref, far_ref, gain_ref, *outs):
    hi_ref, lo_ref = outs[-2:]
    outs = outs[:-2]
    tokens = own_ref.shape[0]
    both = 2 * tokens
    slots = count * 2 * capacity
    lane = lax.broadcasted_iota(jnp.int32, (both, 128), 1)
    tok = lax.broadcasted_iota(jnp.int32, (both, 1), 0)
    side = jnp.where(tok >= tokens, 1, 0)
    hits = [(rel_ref[:, r : r + 1] == lane).astype(F32) for r in range(2)]
    i = lax.broadcasted_iota(jnp.int32, (both, both), 0)
    j = lax.broadcasted_iota(jnp.int32, (both, both), 1)
    earlier = ((j < i) & ((i < tokens) | (j >= tokens))).astype(F32)
    before = jnp.dot(earlier.astype(BF), (hits[0] + hits[1]).astype(BF), preferred_element_type=F32)
    slot_lane = lax.broadcasted_iota(jnp.int32, (both, slots), 1)
    place = jnp.zeros((both, slots), F32)
    weight = jnp.zeros((both, slots), F32)
    for r in range(2):
        slot = jnp.sum(before * hits[r], axis=1, keepdims=True).astype(jnp.int32)
        target = rel_ref[:, r : r + 1] * (2 * capacity) + side * capacity + slot
        here = target == slot_lane
        place = place + jnp.where(here, 1.0, 0.0)
        weight = weight + jnp.where(here, rw_ref[:, r : r + 1], 0.0)
    hi = weight.astype(BF)
    hi_ref[...] = hi
    lo_ref[...] = (weight - hi.astype(F32)).astype(BF)
    placing = place.T.astype(BF)
    normed = []
    for ref in (own_ref, far_ref):
        x = ref[...].astype(F32)
        centered = x - jnp.mean(x, axis=-1, keepdims=True)
        variance = jnp.mean(centered * centered, axis=-1, keepdims=True)
        normed.append((centered * lax.rsqrt(variance + 1e-05) * gain_ref[...]).astype(BF))
    normed = jnp.concatenate(normed, axis=0)
    width = normed.shape[1]
    step = 512
    for c in range(0, width, step):
        y = jnp.dot(placing, normed[:, c : c + step], preferred_element_type=F32).astype(BF)
        at = 0
        for out in outs:
            size = out.shape[0]
            out[:, c : c + step] = y[at : at + size, :]
            at += size


def expert_kernel(sizes, chunk, *refs):
    n = len(sizes)
    ins = refs[:n]
    wg_hbm, wu_hbm, wd_hbm = refs[n : n + 3]
    outs = refs[n + 3 : 2 * n + 3]
    x, wg, wu, wd, y, in_sem, w_sem, out_sem = refs[2 * n + 3 :]
    starts = [sum(sizes[:i]) for i in range(n)]
    weights = [
        pltpu.make_async_copy(a, b, w_sem.at[i])
        for i, (a, b) in enumerate(((wg_hbm.at[0], wg), (wu_hbm.at[0], wu), (wd_hbm.at[0], wd)))
    ]
    loads = [
        pltpu.make_async_copy(ins[i], x.at[pl.ds(starts[i], sizes[i])], in_sem.at[i]) for i in range(n)
    ]
    stores = [
        pltpu.make_async_copy(y.at[pl.ds(starts[i], sizes[i])], outs[i], out_sem.at[i]) for i in range(n)
    ]
    weights[0].start()
    loads[0].start()
    weights[1].start()
    for load in loads[1:]:
        load.start()
    weights[2].start()
    loaded, stored = 0, 0
    total = sum(sizes)
    for at in range(0, total, chunk):
        while loaded < n and starts[loaded] < at + chunk:
            loads[loaded].wait()
            loaded += 1
        if at == 0:
            weights[0].wait()
            weights[1].wait()
        rows = x[at : at + chunk, :]
        gate = jnp.dot(rows, wg[...], preferred_element_type=F32)
        up = jnp.dot(rows, wu[...], preferred_element_type=F32)
        hidden = (gate * up / (1.0 + jnp.exp(-gate))).astype(BF)
        if at == 0:
            weights[2].wait()
        width = wd.shape[1]
        for c in range(0, width, 1024):
            y[at : at + chunk, c : c + 1024] = jnp.dot(
                hidden, wd[:, c : c + 1024], preferred_element_type=F32
            ).astype(BF)
        while stored < n and starts[stored] + sizes[stored] <= at + chunk:
            stores[stored].start()
            stored += 1
    for store in stores:
        store.wait()


def combine_kernel(hi_ref, lo_ref, *refs):
    ins, (own_ref, far_ref) = refs[:-2], refs[-2:]
    tokens = own_ref.shape[0]
    width = own_ref.shape[1]
    for c in range(0, width, 512):
        rows = jnp.concatenate([ref[:, c : c + 512] for ref in ins], axis=0)
        total = jnp.dot(hi_ref[...], rows, preferred_element_type=F32)
        total = total + jnp.dot(lo_ref[...], rows, preferred_element_type=F32)
        own_ref[:, c : c + 512] = total[:tokens]
        far_ref[:, c : c + 512] = total[tokens:].astype(BF)


def cut(array, count):
    size = array.shape[0] // count
    return [array[i * size : (i + 1) * size] for i in range(count)]


def experts_out(expert_input, norm_gain, routes, route_weights):
    tokens, width = expert_input.shape
    count = lax.axis_size("ep")
    half = lax.axis_size("tp") // 2
    capacity = 3 * tokens * routes.shape[1] // (2 * count)
    aligned = 2 * capacity % 16 == 0
    far = swap(expert_input, "tp", half)
    both_routes = jnp.concatenate([routes, swap(routes, "tp", half)], axis=0)
    both_weights = jnp.concatenate([route_weights, swap(route_weights, "tp", half)], axis=0)
    rel = (both_routes - lax.axis_index("ep") + count) % count
    slots = count * 2 * capacity
    sizes = [2 * capacity] * count if aligned else [slots]
    results = pl.pallas_call(
        functools.partial(prep_kernel, count, capacity),
        out_shape=[jax.ShapeDtypeStruct((s, width), BF) for s in sizes]
        + [jax.ShapeDtypeStruct((2 * tokens, slots), BF)] * 2,
        compiler_params=params(40),
        cost_estimate=cost(4e9, 6 << 20),
    )(rel, both_weights, expert_input, far, norm_gain.reshape(1, width))
    blocks = results[:-2]
    if not aligned:
        blocks = cut(blocks[0], count)
    return blocks, results[-2], results[-1], aligned


def experts_mid(blocks, w_gate, w_up, w_down, aligned):
    count = len(blocks)
    arrived = [blocks[0]] + [shift(blocks[d], "ep", d) for d in range(1, count)]
    if not aligned:
        arrived = [jnp.concatenate(arrived, axis=0)]
    near = [swap(block, "tp", 1) for block in arrived]
    pieces = near + arrived
    sizes = [p.shape[0] for p in pieces]
    total = sum(sizes)
    width = pieces[0].shape[1]
    hidden = w_gate.shape[2]
    hbm = pl.BlockSpec(memory_space=pl.ANY)
    outs = pl.pallas_call(
        functools.partial(expert_kernel, sizes, total // 4),
        in_specs=[hbm] * (len(pieces) + 3),
        out_specs=[hbm] * len(pieces),
        out_shape=[jax.ShapeDtypeStruct(p.shape, BF) for p in pieces],
        scratch_shapes=[
            VM((total, width), BF),
            VM((width, hidden), BF),
            VM((width, hidden), BF),
            VM((hidden, width), BF),
            VM((total, width), BF),
            pltpu.SemaphoreType.DMA((len(pieces),)),
            pltpu.SemaphoreType.DMA((3,)),
            pltpu.SemaphoreType.DMA((len(pieces),)),
        ],
        compiler_params=params(44),
        cost_estimate=cost(6 * total * width * hidden, 3 * 2 * width * hidden + 4 * total * width),
    )(*pieces, w_gate, w_up, w_down)
    k = len(near)
    mine = outs[k:]
    given = [swap(out, "tp", 1) for out in outs[:k]]
    summed = [(a.astype(F32) + b.astype(F32)).astype(BF) for a, b in zip(mine, given)]
    if not aligned:
        summed = cut(summed[0], count)
    return [summed[0]] + [shift(summed[d], "ep", -d) for d in range(1, count)]


def experts_end(returned, hi, lo, tokens, aligned):
    half = lax.axis_size("tp") // 2
    width = returned[0].shape[1]
    if not aligned:
        returned = [jnp.concatenate(returned, axis=0)]
    own, far = pl.pallas_call(
        combine_kernel,
        out_shape=[
            jax.ShapeDtypeStruct((tokens, width), F32),
            jax.ShapeDtypeStruct((tokens, width), BF),
        ],
        compiler_params=params(40),
        cost_estimate=cost(2e9, 6 << 20),
    )(hi, lo, *returned)
    return (own + swap(far, "tp", half).astype(F32)).astype(BF)


def per_device(
    query,
    keys,
    values,
    gate_pre,
    log_decay,
    out_weight,
    expert_input,
    norm_gain,
    routes,
    route_weights,
    w_gate,
    w_up,
    w_down,
):
    rows = query.shape[0]
    heads = log_decay.shape[0]
    dk = query.shape[1] // heads
    block = 256
    blocks, hi, lo, aligned = experts_out(expert_input, norm_gain, routes, route_weights)
    cos, sin, run, runt = mixer_tables(rows, dk, log_decay, block)
    packed = mixer_state(keys, values, cos, sin, run, block)
    incoming = incoming_state(packed, heads)
    gated = mixer_gated(query, keys, values, gate_pre, cos, sin, run, runt, incoming, block)
    mixed = project(gated, out_weight)
    returned = experts_mid(blocks, w_gate, w_up, w_down, aligned)
    moe_out = experts_end(returned, hi, lo, expert_input.shape[0], aligned)
    return (mixed, moe_out)


def solution(mesh):
    placed = (
        P("ep", "tp"),
        P("ep", "tp"),
        P("ep", "tp"),
        P("ep", "tp"),
        P("tp", "ep"),
        P(None, "tp"),
        P(("ep", "tp"), None),
        P(),
        P(("ep", "tp"), None),
        P(("ep", "tp"), None),
        P("ep", None, "tp"),
        P("ep", None, "tp"),
        P("ep", "tp", None),
    )
    return jax.shard_map(
        per_device,
        mesh=mesh,
        in_specs=placed,
        out_specs=(P("ep", "tp"), P(("ep", "tp"), None)),
        check_vma=False,
    )
```

```python
import functools
import jax
import jax.numpy as jnp
from jax import lax
from jax.experimental import pallas as pl
from jax.experimental.pallas import tpu as pltpu
from jax.sharding import PartitionSpec as P

BF = jnp.bfloat16
F32 = jnp.float32
VM = pltpu.VMEM


def cost(flops, moved, trans=0):
    return pl.CostEstimate(flops=int(flops), bytes_accessed=int(moved), transcendentals=int(trans))


def params(mib=48, **more):
    return pltpu.CompilerParams(vmem_limit_bytes=mib * 1024 * 1024, **more)


def swap(array, axis, bit):
    size = lax.axis_size(axis)
    return lax.ppermute(array, axis, [(i, i ^ bit) for i in range(size)])


def shift(array, axis, step):
    size = lax.axis_size(axis)
    return lax.ppermute(array, axis, [(i, (i + step) % size) for i in range(size)])


def turn(x, cos_ref, sin_ref, head_dim):
    width = x.shape[1]
    half = head_dim // 2
    lane = lax.broadcasted_iota(jnp.int32, x.shape, 1)
    first = lane % head_dim < half
    other = jnp.where(first, pltpu.roll(x, width - half, 1), pltpu.roll(x, half, 1))
    reps = width // cos_ref.shape[1]
    cos = jnp.concatenate([cos_ref[...]] * reps, axis=1)
    sin = jnp.concatenate([sin_ref[...]] * reps, axis=1)
    return x * cos + other * sin


def next_state(state, kt, value, run_row, closing):
    scaled = (kt * jnp.exp(closing - run_row)).astype(BF)
    return state * jnp.exp(closing) + jnp.dot(scaled, value, preferred_element_type=F32)


def state_kernel(heads, dk, dv, k_ref, v_ref, cos_ref, sin_ref, run_ref, out_ref, state, total):
    b = pl.program_id(0)

    @pl.when(b == 0)
    def _():
        state[...] = jnp.zeros_like(state)
        total[...] = jnp.zeros_like(total)

    kt = (turn(k_ref[...].astype(F32), cos_ref, sin_ref, dk) * dk ** (-0.5)).T
    width = run_ref.shape[2]
    for h in range(heads):
        run_row = run_ref[0, h : h + 1, :]
        closing = run_row[:, width - 1 : width]
        rows = slice(h * dk, (h + 1) * dk)
        state[rows, :] = next_state(
            state[rows, :], kt[rows, :], v_ref[:, h * dv : (h + 1) * dv], run_row, closing
        )
        total[h : h + 1, :] = total[h : h + 1, :] + closing

    @pl.when(b == pl.num_programs(0) - 1)
    def _():
        out_ref[0 : heads * dk, :] = state[...].astype(BF)
        out_ref[heads * dk :, :] = jnp.exp(total[...]).astype(BF)


def mix_kernel(
    heads, dk, dv, q_ref, k_ref, v_ref, g_ref, cos_ref, sin_ref, run_ref, runt_ref, in_ref, out_ref, state
):
    b = pl.program_id(0)

    @pl.when(b == 0)
    def _():
        state[...] = in_ref[...]

    q = turn(q_ref[...].astype(F32), cos_ref, sin_ref, dk)
    kt = (turn(k_ref[...].astype(F32), cos_ref, sin_ref, dk) * dk ** (-0.5)).T
    ktb = kt.astype(BF)
    width = q.shape[0]
    row = lax.broadcasted_iota(jnp.int32, (width, width), 0)
    col = lax.broadcasted_iota(jnp.int32, (width, width), 1)
    causal = row >= col
    for h in range(heads):
        run_row = run_ref[0, h : h + 1, :]
        run_col = runt_ref[:, h : h + 1]
        closing = run_row[:, width - 1 : width]
        rows = slice(h * dk, (h + 1) * dk)
        qh = q[:, rows]
        vh = v_ref[:, h * dv : (h + 1) * dv]
        weights = jnp.where(causal, jnp.exp(jnp.where(causal, run_col - run_row, 0.0)), 0.0)
        scores = jnp.dot(qh.astype(BF), ktb[rows, :], preferred_element_type=F32) * weights
        out = jnp.dot(scores.astype(BF), vh, preferred_element_type=F32)
        carried = state[rows, :]
        out = out + jnp.dot(
            (qh * jnp.exp(run_col)).astype(BF), carried.astype(BF), preferred_element_type=F32
        )
        state[rows, :] = next_state(carried, kt[rows, :], vh, run_row, closing)
        centered = out - jnp.mean(out, axis=-1, keepdims=True)
        variance = jnp.mean(centered * centered, axis=-1, keepdims=True)
        gate = g_ref[:, h * dv : (h + 1) * dv].astype(F32)
        act = gate / (1.0 + jnp.exp(-gate))
        out_ref[:, h * dv : (h + 1) * dv] = (act * (centered * lax.rsqrt(variance + 1e-06))).astype(BF)


def project_kernel(where_ref, a_ref, b_ref, c_ref, d_ref, w_ref, out_ref):
    depth = a_ref.shape[1]
    total = None
    for j, ref in enumerate((a_ref, b_ref, c_ref, d_ref)):
        start = pl.multiple_of(where_ref[j] * depth, depth)
        term = jnp.dot(ref[...], w_ref[pl.ds(start, depth), :], preferred_element_type=F32)
        total = term if total is None else total + term
    out_ref[...] = total.astype(BF)


def mixer_tables(rows, dk, log_decay, block):
    heads = log_decay.shape[0]
    offset = lax.axis_index("ep") * rows
    position = (offset + jnp.arange(rows, dtype=jnp.int32)).astype(F32)
    inverse = 1.0 / 10000.0 ** jnp.linspace(0.0, 1.0, dk // 2, dtype=F32)
    angles = position[:, None] * inverse[None, :]
    cos = jnp.cos(angles)
    sin = jnp.sin(angles)
    reps = 128 // dk
    cos = jnp.concatenate([cos, cos] * reps, axis=1)
    sin = jnp.concatenate([-sin, sin] * reps, axis=1)
    run = jnp.cumsum(log_decay.reshape(heads, rows // block, block), axis=2)
    return cos, sin, run.transpose(1, 0, 2), run.reshape(heads, rows).T


def mixer_state(keys, values, cos, sin, run, block):
    rows = keys.shape[0]
    heads = run.shape[1]
    dk, dv = keys.shape[1] // heads, values.shape[1] // heads
    by_row = lambda b: (b, 0)
    return pl.pallas_call(
        functools.partial(state_kernel, heads, dk, dv),
        grid=(rows // block,),
        in_specs=[
            pl.BlockSpec((block, heads * dk), by_row),
            pl.BlockSpec((block, heads * dv), by_row),
            pl.BlockSpec((block, cos.shape[1]), by_row),
            pl.BlockSpec((block, cos.shape[1]), by_row),
            pl.BlockSpec((1, heads, block), lambda b: (b, 0, 0)),
        ],
        out_specs=pl.BlockSpec((heads * dk + 16, dv), lambda b: (0, 0)),
        out_shape=jax.ShapeDtypeStruct((heads * dk + 16, dv), BF),
        scratch_shapes=[VM((heads * dk, dv), F32), VM((16, dv), F32)],
        compiler_params=params(16),
        cost_estimate=cost(2 * rows * heads * dk * dv, 4 << 20),
    )(keys, values, cos, sin, run)


def spread_kernel(count, x_ref, out_ref, send_sem, recv_sem):
    me = lax.axis_index("ep")
    barrier = pltpu.get_barrier_semaphore()
    for d in range(1, count):
        pl.semaphore_signal(
            barrier, inc=1, device_id={"ep": (me + d) % count}, device_id_type=pl.DeviceIdType.MESH
        )
    pl.semaphore_wait(barrier, count - 1)
    copies = []
    for d in range(1, count):
        copies.append(
            pltpu.make_async_remote_copy(
                src_ref=x_ref,
                dst_ref=out_ref.at[d - 1],
                send_sem=send_sem.at[d - 1],
                recv_sem=recv_sem.at[d - 1],
                device_id={"ep": (me + d) % count},
                device_id_type=pl.DeviceIdType.MESH,
            )
        )
        copies[-1].start()
    for copy in copies:
        copy.wait()


def incoming_state(packed, heads):
    count = lax.axis_size("ep")
    me = lax.axis_index("ep")
    size = packed.shape[0] - 16
    dk = size // heads
    parts = pl.pallas_call(
        functools.partial(spread_kernel, count),
        in_specs=[pl.BlockSpec(memory_space=VM)],
        out_specs=pl.BlockSpec(memory_space=VM),
        out_shape=jax.ShapeDtypeStruct((count - 1,) + packed.shape, BF),
        scratch_shapes=[pltpu.SemaphoreType.DMA((count - 1,))] * 2,
        compiler_params=params(16, collective_id=1, has_side_effects=True),
        cost_estimate=cost(1e9, 8 << 20),
    )(packed)
    state = jnp.zeros((heads, dk, packed.shape[1]), F32)
    factor = jnp.ones((heads, 1, packed.shape[1]), F32)
    for d in range(1, count):
        part = parts[d - 1]
        term = factor * part[:size].astype(F32).reshape(heads, dk, -1)
        state = state + jnp.where(me >= d, term, 0.0)
        factor = factor * part[size : size + heads].astype(F32)[:, None, :]
    return state.reshape(size, packed.shape[1])


def mixer_gated(query, keys, values, gate_pre, cos, sin, run, runt, incoming, block):
    rows = keys.shape[0]
    heads = run.shape[1]
    dk, dv = keys.shape[1] // heads, values.shape[1] // heads
    by_row = lambda b: (b, 0)
    return pl.pallas_call(
        functools.partial(mix_kernel, heads, dk, dv),
        grid=(rows // block,),
        in_specs=[
            pl.BlockSpec((block, heads * dk), by_row),
            pl.BlockSpec((block, heads * dk), by_row),
            pl.BlockSpec((block, heads * dv), by_row),
            pl.BlockSpec((block, heads * dv), by_row),
            pl.BlockSpec((block, cos.shape[1]), by_row),
            pl.BlockSpec((block, cos.shape[1]), by_row),
            pl.BlockSpec((1, heads, block), lambda b: (b, 0, 0)),
            pl.BlockSpec((block, heads), by_row),
            pl.BlockSpec((heads * dk, dv), lambda b: (0, 0)),
        ],
        out_specs=pl.BlockSpec((block, heads * dv), by_row),
        out_shape=jax.ShapeDtypeStruct((rows, heads * dv), BF),
        scratch_shapes=[VM((heads * dk, dv), F32)],
        compiler_params=params(24),
        cost_estimate=cost(6e9, 8 << 20),
    )(query, keys, values, gate_pre, cos, sin, run, runt, incoming)


def project(gated, out_weight):
    half = lax.axis_size("tp") // 2
    me = lax.axis_index("tp")
    far = swap(gated, "tp", half)
    near = swap(gated, "tp", 1)
    both = swap(far, "tp", 1)
    where = jnp.stack([me, me ^ half, me ^ 1, me ^ half ^ 1]).astype(jnp.int32)
    rows, depth = gated.shape
    width = out_weight.shape[1]
    tile = 256
    spec = pl.BlockSpec((tile, depth), lambda i, where: (i, 0))
    return pl.pallas_call(
        project_kernel,
        grid_spec=pltpu.PrefetchScalarGridSpec(
            num_scalar_prefetch=1,
            grid=(rows // tile,),
            in_specs=[spec] * 4 + [pl.BlockSpec(out_weight.shape, lambda i, where: (0, 0))],
            out_specs=pl.BlockSpec((tile, width), lambda i, where: (i, 0)),
        ),
        out_shape=jax.ShapeDtypeStruct((rows, width), BF),
        compiler_params=params(32),
        cost_estimate=cost(2 * rows * depth * 4 * width, 12 << 20),
    )(where, gated, far, near, both, out_weight)


def prep_kernel(count, capacity, rel_ref, rw_ref, own_ref, far_ref, gain_ref, *outs):
    hi_ref, lo_ref = outs[-2:]
    outs = outs[:-2]
    tokens = own_ref.shape[0]
    both = 2 * tokens
    slots = count * 2 * capacity
    lane = lax.broadcasted_iota(jnp.int32, (both, 128), 1)
    tok = lax.broadcasted_iota(jnp.int32, (both, 1), 0)
    side = jnp.where(tok >= tokens, 1, 0)
    hits = [(rel_ref[:, r : r + 1] == lane).astype(F32) for r in range(2)]
    i = lax.broadcasted_iota(jnp.int32, (both, both), 0)
    j = lax.broadcasted_iota(jnp.int32, (both, both), 1)
    earlier = ((j < i) & ((i < tokens) | (j >= tokens))).astype(F32)
    before = jnp.dot(earlier.astype(BF), (hits[0] + hits[1]).astype(BF), preferred_element_type=F32)
    slot_lane = lax.broadcasted_iota(jnp.int32, (both, slots), 1)
    place = jnp.zeros((both, slots), F32)
    weight = jnp.zeros((both, slots), F32)
    for r in range(2):
        slot = jnp.sum(before * hits[r], axis=1, keepdims=True).astype(jnp.int32)
        target = rel_ref[:, r : r + 1] * (2 * capacity) + side * capacity + slot
        here = target == slot_lane
        place = place + jnp.where(here, 1.0, 0.0)
        weight = weight + jnp.where(here, rw_ref[:, r : r + 1], 0.0)
    hi = weight.astype(BF)
    hi_ref[...] = hi
    lo_ref[...] = (weight - hi.astype(F32)).astype(BF)
    placing = place.T.astype(BF)
    normed = []
    for ref in (own_ref, far_ref):
        x = ref[...].astype(F32)
        centered = x - jnp.mean(x, axis=-1, keepdims=True)
        variance = jnp.mean(centered * centered, axis=-1, keepdims=True)
        normed.append((centered * lax.rsqrt(variance + 1e-05) * gain_ref[...]).astype(BF))
    normed = jnp.concatenate(normed, axis=0)
    width = normed.shape[1]
    step = 512
    for c in range(0, width, step):
        y = jnp.dot(placing, normed[:, c : c + step], preferred_element_type=F32).astype(BF)
        at = 0
        for out in outs:
            size = out.shape[0]
            out[:, c : c + step] = y[at : at + size, :]
            at += size


def expert_kernel(sizes, chunk, *refs):
    n = len(sizes)
    ins = refs[:n]
    wg_hbm, wu_hbm, wd_hbm = refs[n : n + 3]
    outs = refs[n + 3 : 2 * n + 3]
    x, wg, wu, wd, y, in_sem, w_sem, out_sem = refs[2 * n + 3 :]
    starts = [sum(sizes[:i]) for i in range(n)]
    weights = [
        pltpu.make_async_copy(a, b, w_sem.at[i])
        for i, (a, b) in enumerate(((wg_hbm.at[0], wg), (wu_hbm.at[0], wu), (wd_hbm.at[0], wd)))
    ]
    loads = [
        pltpu.make_async_copy(ins[i], x.at[pl.ds(starts[i], sizes[i])], in_sem.at[i]) for i in range(n)
    ]
    stores = [
        pltpu.make_async_copy(y.at[pl.ds(starts[i], sizes[i])], outs[i], out_sem.at[i]) for i in range(n)
    ]
    weights[0].start()
    loads[0].start()
    weights[1].start()
    for load in loads[1:]:
        load.start()
    weights[2].start()
    loaded, stored = 0, 0
    total = sum(sizes)
    for at in range(0, total, chunk):
        while loaded < n and starts[loaded] < at + chunk:
            loads[loaded].wait()
            loaded += 1
        if at == 0:
            weights[0].wait()
            weights[1].wait()
        rows = x[at : at + chunk, :]
        gate = jnp.dot(rows, wg[...], preferred_element_type=F32)
        up = jnp.dot(rows, wu[...], preferred_element_type=F32)
        hidden = (gate * up / (1.0 + jnp.exp(-gate))).astype(BF)
        if at == 0:
            weights[2].wait()
        width = wd.shape[1]
        for c in range(0, width, 1024):
            y[at : at + chunk, c : c + 1024] = jnp.dot(
                hidden, wd[:, c : c + 1024], preferred_element_type=F32
            ).astype(BF)
        while stored < n and starts[stored] + sizes[stored] <= at + chunk:
            stores[stored].start()
            stored += 1
    for store in stores:
        store.wait()


def combine_kernel(hi_ref, lo_ref, *refs):
    ins, (own_ref, far_ref) = refs[:-2], refs[-2:]
    tokens = own_ref.shape[0]
    width = own_ref.shape[1]
    for c in range(0, width, 512):
        rows = jnp.concatenate([ref[:, c : c + 512] for ref in ins], axis=0)
        total = jnp.dot(hi_ref[...], rows, preferred_element_type=F32)
        total = total + jnp.dot(lo_ref[...], rows, preferred_element_type=F32)
        own_ref[:, c : c + 512] = total[:tokens]
        far_ref[:, c : c + 512] = total[tokens:].astype(BF)


def return_kernel(count, *refs):
    near, mine = refs[:count], refs[count : 2 * count]
    outs = refs[2 * count : 3 * count]
    got, summed, near_send, near_recv, far_send, far_recv = refs[3 * count :]
    me = lax.axis_index("ep")
    sibling = {"tp": lax.axis_index("tp") ^ 1}
    mesh_id = pl.DeviceIdType.MESH
    barrier = pltpu.get_barrier_semaphore()
    pl.semaphore_signal(barrier, inc=1, device_id=sibling, device_id_type=mesh_id)
    for d in range(1, count):
        pl.semaphore_signal(
            barrier, inc=1, device_id={"ep": (me + d) % count}, device_id_type=mesh_id
        )
    pl.semaphore_wait(barrier, count)
    order = list(range(1, count)) + [0]
    across = {}
    for d in order:
        across[d] = pltpu.make_async_remote_copy(
            src_ref=near[d],
            dst_ref=got.at[d],
            send_sem=near_send.at[d],
            recv_sem=near_recv.at[d],
            device_id=sibling,
            device_id_type=mesh_id,
        )
        across[d].start()
    back = {}
    for k, d in enumerate(order):
        across[d].wait_recv()
        total = (mine[d][...].astype(F32) + got[d].astype(F32)).astype(BF)
        if d == 0:
            outs[0][...] = total
        else:
            summed[d - 1] = total
        if k:
            e = order[k - 1]
            back[e] = pltpu.make_async_remote_copy(
                src_ref=summed.at[e - 1],
                dst_ref=outs[e],
                send_sem=far_send.at[e - 1],
                recv_sem=far_recv.at[e - 1],
                device_id={"ep": (me + count - e) % count},
                device_id_type=mesh_id,
            )
            back[e].start()
    for d in order:
        across[d].wait_send()
    for copy in back.values():
        copy.wait()


def give_back(near, mine):
    count = len(near)
    shape = near[0].shape
    vmem = pl.BlockSpec(memory_space=VM)
    return pl.pallas_call(
        functools.partial(return_kernel, count),
        in_specs=[vmem] * (2 * count),
        out_specs=[vmem] * count,
        out_shape=[jax.ShapeDtypeStruct(shape, BF)] * count,
        scratch_shapes=[
            VM((count,) + shape, BF),
            VM((count - 1,) + shape, BF),
            pltpu.SemaphoreType.DMA((count,)),
            pltpu.SemaphoreType.DMA((count,)),
            pltpu.SemaphoreType.DMA((count - 1,)),
            pltpu.SemaphoreType.DMA((count - 1,)),
        ],
        compiler_params=params(32, collective_id=2, has_side_effects=True),
        cost_estimate=cost(2e10, 60 << 20),
    )(*near, *mine)


def cut(array, count):
    size = array.shape[0] // count
    return [array[i * size : (i + 1) * size] for i in range(count)]


def experts_out(expert_input, norm_gain, routes, route_weights):
    tokens, width = expert_input.shape
    count = lax.axis_size("ep")
    half = lax.axis_size("tp") // 2
    capacity = 3 * tokens * routes.shape[1] // (2 * count)
    aligned = 2 * capacity % 16 == 0
    far = swap(expert_input, "tp", half)
    top = routes.shape[1]
    pairs = jnp.concatenate([routes.astype(F32), route_weights], axis=1)
    pairs = jnp.concatenate([pairs, swap(pairs, "tp", half)], axis=0)
    both_routes, both_weights = pairs[:, :top].astype(jnp.int32), pairs[:, top:]
    rel = (both_routes - lax.axis_index("ep") + count) % count
    slots = count * 2 * capacity
    sizes = [2 * capacity] * count if aligned else [slots]
    results = pl.pallas_call(
        functools.partial(prep_kernel, count, capacity),
        out_shape=[jax.ShapeDtypeStruct((s, width), BF) for s in sizes]
        + [jax.ShapeDtypeStruct((2 * tokens, slots), BF)] * 2,
        compiler_params=params(40),
        cost_estimate=cost(4e9, 6 << 20),
    )(rel, both_weights, expert_input, far, norm_gain.reshape(1, width))
    blocks = results[:-2]
    if not aligned:
        blocks = cut(blocks[0], count)
    return blocks, results[-2], results[-1], aligned


def experts_mid(blocks, w_gate, w_up, w_down, aligned):
    count = len(blocks)
    arrived = [blocks[0]] + [shift(blocks[d], "ep", d) for d in range(1, count)]
    if not aligned:
        arrived = [jnp.concatenate(arrived, axis=0)]
    near = [swap(block, "tp", 1) for block in arrived]
    pieces = near + arrived
    sizes = [p.shape[0] for p in pieces]
    total = sum(sizes)
    width = pieces[0].shape[1]
    hidden = w_gate.shape[2]
    hbm = pl.BlockSpec(memory_space=pl.ANY)
    outs = pl.pallas_call(
        functools.partial(expert_kernel, sizes, total // 4),
        in_specs=[hbm] * (len(pieces) + 3),
        out_specs=[hbm] * len(pieces),
        out_shape=[jax.ShapeDtypeStruct(p.shape, BF) for p in pieces],
        scratch_shapes=[
            VM((total, width), BF),
            VM((width, hidden), BF),
            VM((width, hidden), BF),
            VM((hidden, width), BF),
            VM((total, width), BF),
            pltpu.SemaphoreType.DMA((len(pieces),)),
            pltpu.SemaphoreType.DMA((3,)),
            pltpu.SemaphoreType.DMA((len(pieces),)),
        ],
        compiler_params=params(44),
        cost_estimate=cost(6 * total * width * hidden, 3 * 2 * width * hidden + 4 * total * width),
    )(*pieces, w_gate, w_up, w_down)
    k = len(near)
    mine = outs[k:]
    if aligned:
        return give_back(outs[:k], mine)
    given = [swap(out, "tp", 1) for out in outs[:k]]
    summed = (mine[0].astype(F32) + given[0].astype(F32)).astype(BF)
    summed = cut(summed, count)
    return [summed[0]] + [shift(summed[d], "ep", -d) for d in range(1, count)]


def experts_end(returned, hi, lo, tokens, aligned):
    half = lax.axis_size("tp") // 2
    width = returned[0].shape[1]
    if not aligned:
        returned = [jnp.concatenate(returned, axis=0)]
    own, far = pl.pallas_call(
        combine_kernel,
        out_shape=[
            jax.ShapeDtypeStruct((tokens, width), F32),
            jax.ShapeDtypeStruct((tokens, width), BF),
        ],
        compiler_params=params(40),
        cost_estimate=cost(2e9, 6 << 20),
    )(hi, lo, *returned)
    return (own + swap(far, "tp", half).astype(F32)).astype(BF)


def per_device(
    query,
    keys,
    values,
    gate_pre,
    log_decay,
    out_weight,
    expert_input,
    norm_gain,
    routes,
    route_weights,
    w_gate,
    w_up,
    w_down,
):
    rows = query.shape[0]
    heads = log_decay.shape[0]
    dk = query.shape[1] // heads
    block = 256
    blocks, hi, lo, aligned = experts_out(expert_input, norm_gain, routes, route_weights)
    cos, sin, run, runt = mixer_tables(rows, dk, log_decay, block)
    packed = mixer_state(keys, values, cos, sin, run, block)
    incoming = incoming_state(packed, heads)
    gated = mixer_gated(query, keys, values, gate_pre, cos, sin, run, runt, incoming, block)
    mixed = project(gated, out_weight)
    returned = experts_mid(blocks, w_gate, w_up, w_down, aligned)
    moe_out = experts_end(returned, hi, lo, expert_input.shape[0], aligned)
    return (mixed, moe_out)


def solution(mesh):
    placed = (
        P("ep", "tp"),
        P("ep", "tp"),
        P("ep", "tp"),
        P("ep", "tp"),
        P("tp", "ep"),
        P(None, "tp"),
        P(("ep", "tp"), None),
        P(),
        P(("ep", "tp"), None),
        P(("ep", "tp"), None),
        P("ep", None, "tp"),
        P("ep", None, "tp"),
        P("ep", "tp", None),
    )
    return jax.shard_map(
        per_device,
        mesh=mesh,
        in_specs=placed,
        out_specs=(P("ep", "tp"), P(("ep", "tp"), None)),
        check_vma=False,
    )
```
